256 devices in a mesh: sp: 64 (over z, x, core), tp: 4 (over y).
Axes of the slice: x: 4, y: 4, z: 8, core: 2. Of those that a mesh axis runs over, the one named last changes fastest.
Arguments:
- stream: bfloat16 [32768, 2048], P(('sp', 'tp')), may hold values from -6 to 6
- broad_queries: bfloat16 [32768, 512], P('sp', 'tp'), may hold values from -6 to 6
- broad_keys: bfloat16 [32768, 512], P('sp', 'tp'), may hold values from -6 to 6
- broad_values: bfloat16 [32768, 1024], P('sp', 'tp'), may hold values from -6 to 6
- broad_output_gate: bfloat16 [32768, 1024], P('sp', 'tp'), may hold values from -6 to 6
- broad_input_gate: float32 [4, 32768], P('tp', 'sp'), may hold values from -6 to 130
- broad_forget_logits: float32 [4, 32768], P('tp', 'sp'), may hold values from 0 to 20
- broad_forget_boost: float32 [4, 32768], P('tp', 'sp'), may hold values from -1 to 0
- slim_queries: bfloat16 [32768, 512], P('sp', 'tp'), may hold values from -6 to 6
- slim_keys: bfloat16 [32768, 512], P('sp', 'tp'), may hold values from -6 to 6
- slim_values: bfloat16 [32768, 1024], P('sp', 'tp'), may hold values from -6 to 6
- slim_output_gate: bfloat16 [32768, 1024], P('sp', 'tp'), may hold values from -6 to 6
- slim_input_gate: float32 [8, 32768], P('tp', 'sp'), may hold values from -6 to 130
- slim_forget_logits: float32 [8, 32768], P('tp', 'sp'), may hold values from 0 to 20
- slim_forget_boost: float32 [8, 32768], P('tp', 'sp'), may hold values from -1 to 0
- broad_output_weight: bfloat16 [1024, 2048], P('tp'), may hold values from -0.125 to 0.125
- slim_output_weight: bfloat16 [1024, 2048], P('tp'), may hold values from -0.125 to 0.125
- expert_norm_gain: float32 [2048], replicated, may hold values from 0.1 to 1.9
- routes: int32 [32768, 2], P('sp'), may hold values from 0 to 63, all different within a row; in each aligned block of 128 rows (0 to 127, 128 to 255, ...) at most 8 rows name the same one
- routing_weight: float32 [32768, 2], P(('sp', 'tp')), may hold values from 0.2 to 1
- expert_gate_weight: bfloat16 [64, 2048, 2048], P('sp', None, 'tp'), may hold values from -0.375 to 0.375
- expert_linear_weight: bfloat16 [64, 2048, 2048], P('sp', None, 'tp'), may hold values from -0.375 to 0.375
- expert_down_weight: bfloat16 [64, 2048, 2048], P('sp', 'tp'), may hold values from -0.01953125 to 0.01953125
Outputs:
- block_out: bfloat16 [32768, 2048], P(('sp', 'tp'))
The draws below stay inside these ranges and needn't reach their ends.
Inputs may be any that keep to these rules, and one draw needn't show every extreme that they name: `routes`: in each aligned block of 128 rows, a row names 2 different experts and no expert is named by more than 8 rows; every expert is named somewhere.
All inputs are finite; a program needn't handle non-finite values.
Results may differ from the reference program's by a relative error of at most 0.015.
Values may be sent and summed in bfloat16 or wider, within the bound.
No kernel may reach another device: no remote copies, remote signals or barrier semaphores. Data moves between devices by JAX's collectives and lax.ppermute only.
A program may use at most 128 MiB of HBM per device.

```python
import math
from functools import partial
import jax
import jax.numpy as jnp
import numpy as np
from jax import lax

D = 2048
FF = 2048
BROAD_HEADS = 4
DKA = 128
DVA = 256
SLIM_HEADS = 8
DKB = 64
DVB = 128
TOPK = 2
TOK_DEV = 512
TOKENS = 32768
ROWS = 128
EXPERTS = 64
CAP = 8
N_TP = 4


def input_gate(key, head_total):
    first = jax.random.fold_in(key, 0)
    value_rows = jnp.clip(jax.random.normal(first, (head_total, TOKENS), jnp.float32), -6.0, 6.0)
    return value_rows


def forget_gate(key, head_total):
    first, second, third, fourth = jax.random.split(key, 4)
    share_fast = 0.5
    is_fast = jax.random.uniform(first, (head_total,), jnp.float32) < share_fast
    fast_base = jax.random.uniform(second, (head_total,), jnp.float32, jnp.log(30.0), jnp.log(100.0))
    slow_base = jnp.log(2.0 * TOKENS) * jnp.ones((head_total,), jnp.float32)
    base = jnp.where(is_fast, fast_base, slow_base)
    blocks = TOKENS // TOK_DEV
    shifts = jax.random.uniform(third, (head_total, blocks), jnp.float32, -0.7, 0.7)
    shifts = jnp.repeat(shifts, TOK_DEV, axis=1)
    noise = 0.5 * jax.random.normal(fourth, (head_total, TOKENS), jnp.float32)
    return jnp.clip(base[:, None] + shifts + noise, 0.0, 20.0)


def boost_sample(key, head_total):
    first, second = jax.random.split(key, 2)
    spots = jax.random.randint(first, (head_total, 3), 0, TOKENS)
    losses = jax.random.uniform(second, (head_total, 3), jnp.float32, 0.2, 0.5)
    value_rows = jnp.zeros((head_total, TOKENS), jnp.float32)
    return value_rows.at[jnp.arange(head_total)[:, None], spots].set(jnp.log(1.0 - losses))


def draw_broad_input_gate(key, part):
    return input_gate(jax.random.fold_in(key, 11), BROAD_HEADS)


def draw_slim_input_gate(key, part):
    return input_gate(jax.random.fold_in(key, 12), SLIM_HEADS)


def draw_broad_forget_logits(key, part):
    return forget_gate(jax.random.fold_in(key, 21), BROAD_HEADS)


def draw_slim_forget_logits(key, part):
    return forget_gate(jax.random.fold_in(key, 22), SLIM_HEADS)


def draw_broad_forget_boost(key, part):
    return boost_sample(jax.random.fold_in(key, 31), BROAD_HEADS)


def draw_slim_forget_boost(key, part):
    return boost_sample(jax.random.fold_in(key, 32), SLIM_HEADS)


def levels(rng, shape, shards, smallest, top_value):
    def one(axis_at, shards_of):
        draws = jax.random.uniform(jax.random.fold_in(jax.random.fold_in(rng, 6), axis_at), (shards_of,), jnp.float32, smallest / len(shards), top_value / len(shards))
        return jnp.repeat(jnp.exp(draws), shape[axis_at] // shards_of).reshape((-1,) + (1,) * (len(shape) - axis_at - 1))

    level = one(*shards[0])
    for cut in shards[1:]:
        level = level * one(*cut)
    return level


def routed_block(stream_key, own, number, rows, number_of, top, reach, slope):
    ranking = jax.random.permutation(stream_key, number_of)
    crowded, common = load_shares(number_of, rows * top, reach, slope, True), load_shares(number_of, rows * top, reach, slope, False)
    places = jnp.arange(number_of)

    def named(sizes, turn):
        used = int((sizes > 0).sum())
        fixed = max(1, used // 4)
        passed = fixed + (places - fixed + turn * (used - fixed)) % max(1, number_of - fixed)
        return jnp.zeros((number_of,), jnp.int32).at[ranking[jnp.where(places < fixed, places, passed)]].set(jnp.asarray(sizes, jnp.int32))

    sizes = jnp.where(number % 4 == 0, named(crowded, number // 4), named(common, number - number // 4 - 1))
    mixed = jax.random.permutation(jax.random.fold_in(own, 3), number_of)
    giver, receiver = mixed[0:number_of // 2 * 2:2], mixed[1:number_of // 2 * 2:2]
    room = jnp.minimum(sizes[giver] - 1, reach - sizes[receiver]) // 2
    room = jnp.where((giver == ranking[0]) | (receiver == ranking[0]) | (sizes[receiver] == 0), 0, jnp.maximum(room, 0))
    passed = jax.random.randint(jax.random.fold_in(own, 4), (number_of // 2,), 0, 1 << 20) % (room + 1)
    sizes = sizes.at[giver].add(-passed).at[receiver].add(passed)
    members = jnp.searchsorted(jnp.cumsum(sizes), jnp.arange(rows * top), side="right").astype(jnp.int32)
    grid = members.reshape(top, rows).T
    grid = grid[jax.random.permutation(jax.random.fold_in(own, 1), rows)]
    turn = jax.random.randint(jax.random.fold_in(own, 2), (rows, 1), 0, top)
    return jnp.take_along_axis(grid, (jnp.arange(top)[None, :] + turn) % top, axis=1)


def load_shares(count, total, limit, lean, full):
    loads = [(1 << 20) // math.isqrt(standing ** lean) + 1 for standing in range(1, count + 1)]
    largest = limit if full else min(limit, max(-(-total // count), total * loads[0] // sum(loads)))
    least = 1 if total - largest >= count - 1 else 0
    given, surplus = [largest] + [least] * (count - 1), total - largest - least * (count - 1)
    while surplus > 0:
        movable = [i for i in range(1, count) if given[i] < largest] or [i for i in range(1, count) if given[i] < limit]
        mass, left = sum([loads[i] for i in movable]), surplus
        for i in movable:
            more = min(limit - given[i], max(1, left * loads[i] // mass), surplus)
            given[i] = given[i] + more
            surplus = surplus - more
    return np.array(given)


def gaussian(stream_key, extent, scale, reach, pieces=(), held_as=jnp.bfloat16):
    values = scale * jax.random.normal(stream_key, extent, jnp.float32)
    if pieces:
        values = values * levels(stream_key, extent, pieces, -0.22, 0.18)
    return jnp.clip(values, -reach, reach).astype(held_as)


def setup_inputs(seed: int = 0) -> dict:
    key_list = jax.random.split(jax.random.key(seed), 24)
    stream = gaussian(key_list[0], (TOKENS, D), 1.0, 6.0, ((0, 256),))
    broad_queries = gaussian(key_list[1], (TOKENS, BROAD_HEADS * DKA), 1.0, 6.0, ((0, 64), (1, 4)))
    broad_keys = gaussian(key_list[2], (TOKENS, BROAD_HEADS * DKA), 1.0, 6.0, ((0, 64), (1, 4)))
    broad_values = gaussian(key_list[3], (TOKENS, BROAD_HEADS * DVA), 1.0, 6.0, ((0, 64), (1, 4)))
    broad_output_gate = gaussian(key_list[4], (TOKENS, BROAD_HEADS * DVA), 1.0, 6.0, ((0, 64), (1, 4)))
    broad_input_gate = draw_broad_input_gate(jax.random.fold_in(key_list[23], 71), 0)
    broad_forget_logits = draw_broad_forget_logits(jax.random.fold_in(key_list[23], 71), 0)
    broad_forget_boost = draw_broad_forget_boost(jax.random.fold_in(key_list[23], 71), 0)
    slim_queries = gaussian(key_list[8], (TOKENS, SLIM_HEADS * DKB), 1.0, 6.0, ((0, 64), (1, 4)))
    slim_keys = gaussian(key_list[9], (TOKENS, SLIM_HEADS * DKB), 1.0, 6.0, ((0, 64), (1, 4)))
    slim_values = gaussian(key_list[10], (TOKENS, SLIM_HEADS * DVB), 1.0, 6.0, ((0, 64), (1, 4)))
    slim_output_gate = gaussian(key_list[11], (TOKENS, SLIM_HEADS * DVB), 1.0, 6.0, ((0, 64), (1, 4)))
    slim_input_gate = draw_slim_input_gate(jax.random.fold_in(key_list[23], 71), 0)
    slim_forget_logits = draw_slim_forget_logits(jax.random.fold_in(key_list[23], 71), 0)
    slim_forget_boost = draw_slim_forget_boost(jax.random.fold_in(key_list[23], 71), 0)
    broad_output_weight = gaussian(key_list[15], (BROAD_HEADS * DVA, D), (BROAD_HEADS * DVA + SLIM_HEADS * DVB) ** -0.5, 0.125, ((0, 4),))
    slim_output_weight = gaussian(key_list[16], (SLIM_HEADS * DVB, D), (BROAD_HEADS * DVA + SLIM_HEADS * DVB) ** -0.5, 0.125, ((0, 4),))
    expert_norm_gain = jnp.clip(1.0 + 0.18 * jax.random.normal(key_list[17], (D,), jnp.float32), 0.1, 1.9)
    routes_keys = jax.random.split(jax.random.fold_in(key_list[18], 1), TOKENS // ROWS)
    routes_turns = jax.random.permutation(jax.random.fold_in(key_list[18], 3), TOKENS // ROWS)
    routes = jax.vmap(lambda own, number: routed_block(jax.random.fold_in(key_list[18], 2), own, number, ROWS, EXPERTS, TOPK, CAP, 1))(routes_keys, routes_turns).reshape((TOKENS, TOPK))
    routing_weight = jnp.clip(0.2 + 0.8 * jax.random.uniform(key_list[19], (TOKENS, TOPK), jnp.float32) ** levels(key_list[19], (TOKENS, TOPK), ((0, 256),), -0.2, 0.2), 0.2, 1.0)
    expert_gate_weight = gaussian(key_list[20], (EXPERTS, D, FF), (D // 9) ** -0.5, 0.375, ((0, 64), (2, 4)))
    expert_linear_weight = gaussian(key_list[21], (EXPERTS, D, FF), (D // 9) ** -0.5, 0.375, ((0, 64), (2, 4)))
    expert_down_weight = gaussian(key_list[22], (EXPERTS, FF, D), (FF * 40) ** -0.5, 0.01953125, ((0, 64), (1, 4)))
    return {"stream": stream, "broad_queries": broad_queries, "broad_keys": broad_keys, "broad_values": broad_values, "broad_output_gate": broad_output_gate, "broad_input_gate": broad_input_gate, "broad_forget_logits": broad_forget_logits, "broad_forget_boost": broad_forget_boost, "slim_queries": slim_queries, "slim_keys": slim_keys, "slim_values": slim_values, "slim_output_gate": slim_output_gate, "slim_input_gate": slim_input_gate, "slim_forget_logits": slim_forget_logits, "slim_forget_boost": slim_forget_boost, "broad_output_weight": broad_output_weight, "slim_output_weight": slim_output_weight, "expert_norm_gain": expert_norm_gain, "routes": routes, "routing_weight": routing_weight, "expert_gate_weight": expert_gate_weight, "expert_linear_weight": expert_linear_weight, "expert_down_weight": expert_down_weight}


EPSILON = 1e-06
FLOOR_LOG = -1e+30
LIMIT = 7.0
SLOPE = 1.702
TOP_PRECISION = lax.Precision.HIGHEST

def rounded(value):
    return lax.optimization_barrier(value.astype(jnp.bfloat16)).astype(jnp.float32)

def summarize(key_rows, value_rows, input_gate_log, log_forget):
    key_size = key_rows.shape[2]
    prefix = jnp.cumsum(log_forget, axis=1)
    totals = prefix[:, -1]
    spread = totals[:, None] - prefix + input_gate_log
    local_max = lax.optimization_barrier(jnp.max(spread, axis=1))
    weights = jnp.exp(spread - local_max[:, None])
    scaled = key_rows.astype(jnp.float32) / math.sqrt(key_size)
    weighted_output = rounded(jnp.transpose(weights)[:, :, None] * scaled)
    matrix_memory = jnp.einsum('zqi,zqs->qis', weighted_output, value_rows.astype(jnp.float32), precision=TOP_PRECISION)
    return (totals, local_max, matrix_memory)

def merge_states(earlier, later):
    first_total, first_max, first_memory = earlier
    second_total, second_max, second_memory = later
    new_max = jnp.maximum(second_total + first_max, second_max)
    old_scale = jnp.exp(second_total + first_max - new_max)
    new_scale = jnp.exp(second_max - new_max)
    return (first_total + second_total, new_max, old_scale[:, None, None] * first_memory + new_scale[:, None, None] * second_memory)

def read_out(query_rows, key_rows, value_rows, input_gate_log, log_forget, state):
    matrix_memory, carried_max = state
    key_size = key_rows.shape[2]
    length = query_rows.shape[0]
    prefix = jnp.cumsum(log_forget, axis=1)
    causal = lax.broadcasted_iota(jnp.int32, (length, length), 0) >= lax.broadcasted_iota(jnp.int32, (length, length), 1)
    decays = jnp.where(causal[None], prefix[:, :, None] - prefix[:, None, :] + input_gate_log[:, None, :], -jnp.inf)
    carried_log = prefix + carried_max[:, None]
    row_max = jnp.maximum(carried_log, lax.optimization_barrier(jnp.max(decays, axis=2)))
    widened_query = query_rows.astype(jnp.float32)
    scores = jnp.einsum('thk,shk->hts', widened_query, key_rows.astype(jnp.float32), precision=TOP_PRECISION) / math.sqrt(key_size)
    weights = jnp.exp(decays - row_max[:, :, None]) * scores
    carried_route_weight = jnp.exp(carried_log - row_max)
    memory_numerator = carried_route_weight[:, :, None] * jnp.einsum('ldm,dmb->dlb', widened_query, matrix_memory, precision=TOP_PRECISION)
    return memory_numerator + jnp.einsum('hts,shv->htv', rounded(weights), value_rows.astype(jnp.float32), precision=TOP_PRECISION)

def gate_out(cells, output_gate_logits):
    head_total, length, width = cells.shape
    square = lax.optimization_barrier(jnp.mean(cells * cells, axis=2, keepdims=True))
    normed = cells * lax.rsqrt(square + EPSILON)
    normed = jnp.transpose(normed, (1, 0, 2)).reshape(length, head_total * width)
    return (normed * jax.nn.sigmoid(output_gate_logits.astype(jnp.float32))).astype(jnp.bfloat16)

def run_head_group(query_rows, key_rows, value_rows, output_gate_logits, input_gate_log, forget_logits, forget_boost):
    head_total = input_gate_log.shape[0]
    tokens = query_rows.shape[0]
    blocks = tokens // TOK_DEV
    log_forget = jax.nn.log_sigmoid(forget_logits) + forget_boost
    query_blocks = query_rows.reshape(blocks, TOK_DEV, head_total, -1)
    key_blocks = key_rows.reshape(blocks, TOK_DEV, head_total, -1)
    value_blocks = value_rows.reshape(blocks, TOK_DEV, head_total, -1)
    ingate_blocks = jnp.transpose(input_gate_log.reshape(head_total, blocks, TOK_DEV), (1, 0, 2))
    logf_blocks = jnp.transpose(log_forget.reshape(head_total, blocks, TOK_DEV), (1, 0, 2))
    key_size = query_blocks.shape[3]
    value_size = value_blocks.shape[3]
    start = (jnp.zeros((head_total, key_size, value_size), jnp.float32), jnp.full((head_total,), FLOOR_LOG, jnp.float32))

    def advance(state, inputs):
        query_now, key_now, value_now, ingate_now, logf_now = inputs
        cells = read_out(query_now, key_now, value_now, ingate_now, logf_now, state)
        summary = summarize(key_now, value_now, ingate_now, logf_now)
        matrix_memory, carried_max = state
        merged = merge_states((jnp.zeros((head_total,), jnp.float32), carried_max, matrix_memory), summary)
        return ((merged[2], merged[1]), cells)
    _, cells = lax.scan(advance, start, (query_blocks, key_blocks, value_blocks, ingate_blocks, logf_blocks))
    cells = jnp.transpose(cells, (1, 0, 2, 3)).reshape(head_total, tokens, value_size)
    return gate_out(cells, output_gate_logits)

def slot_table(block_routes, experts, capacity):
    rows, top = block_routes.shape
    entries = rows * top
    flat = block_routes.reshape(entries)
    onehot = (flat[:, None] == jnp.arange(experts, dtype=jnp.int32)[None, :]).astype(jnp.float32)
    lower = (lax.broadcasted_iota(jnp.int32, (entries, entries), 0) > lax.broadcasted_iota(jnp.int32, (entries, entries), 1)).astype(jnp.float32)
    before = jnp.dot(lower, onehot, precision=TOP_PRECISION)
    ranks = lax.optimization_barrier(jnp.sum(before * onehot, axis=1)).astype(jnp.int32)
    slots = flat * capacity + ranks
    matches = slots[None, :] == jnp.arange(experts * capacity, dtype=jnp.int32)[:, None]
    owners = jnp.arange(entries, dtype=jnp.int32) // top
    source = lax.optimization_barrier(jnp.sum(jnp.where(matches, owners[None, :] + 1, 0), axis=1)).astype(jnp.int32) - 1
    return (slots, source)

def reference(stream, broad_queries, broad_keys, broad_values, broad_output_gate, broad_input_gate, broad_forget_logits, broad_forget_boost, slim_queries, slim_keys, slim_values, slim_output_gate, slim_input_gate, slim_forget_logits, slim_forget_boost, broad_output_weight, slim_output_weight, expert_norm_gain, routes, routing_weight, expert_gate_weight, expert_linear_weight, expert_down_weight):
    broad_mixed_output = run_head_group(broad_queries, broad_keys, broad_values, broad_output_gate, broad_input_gate, broad_forget_logits, broad_forget_boost)
    slim_mixed_output = run_head_group(slim_queries, slim_keys, slim_values, slim_output_gate, slim_input_gate, slim_forget_logits, slim_forget_boost)
    broad_cols = broad_mixed_output.shape[1] // N_TP
    slim_cols = slim_mixed_output.shape[1] // N_TP
    head_sum = jnp.zeros(stream.shape, jnp.float32)
    for index in range(N_TP):
        part_value = jnp.dot(broad_mixed_output[:, index * broad_cols:(index + 1) * broad_cols], broad_output_weight[index * broad_cols:(index + 1) * broad_cols], preferred_element_type=jnp.float32)
        part_value = part_value + jnp.dot(slim_mixed_output[:, index * slim_cols:(index + 1) * slim_cols], slim_output_weight[index * slim_cols:(index + 1) * slim_cols], preferred_element_type=jnp.float32)
        head_sum = head_sum + rounded(part_value)
    middle = (stream.astype(jnp.float32) + head_sum).astype(jnp.bfloat16)
    middle_wide = middle.astype(jnp.float32)
    normed = (middle_wide * lax.rsqrt(lax.optimization_barrier(jnp.mean(middle_wide * middle_wide, axis=1, keepdims=True)) + EPSILON) * expert_norm_gain.astype(jnp.float32)).astype(jnp.bfloat16)
    tokens, width = normed.shape
    rows = TOK_DEV // N_TP
    blocks = tokens // rows
    grouped = routes.reshape(blocks, rows, TOPK)
    slots, source = jax.vmap(partial(slot_table, experts=EXPERTS, capacity=CAP))(grouped)
    offsets = jnp.arange(blocks, dtype=jnp.int32)[:, None] * rows
    picks = jnp.where(source < 0, tokens, source + offsets)
    picks = jnp.transpose(picks.reshape(blocks, EXPERTS, CAP), (1, 0, 2)).reshape(EXPERTS, blocks * CAP)
    padded = jnp.concatenate([normed, jnp.zeros((1, width), jnp.bfloat16)], axis=0)
    piece_size = FF // N_TP

    def expert_apply(inputs):
        row_index, gate_weight, lin_weight, down_weight = inputs
        buffer = padded[row_index]
        gate_pre = jnp.dot(buffer, gate_weight, preferred_element_type=jnp.float32)
        lin_pre = jnp.dot(buffer, lin_weight, preferred_element_type=jnp.float32)
        glu = jnp.minimum(gate_pre, LIMIT)
        linear = jnp.clip(lin_pre, -LIMIT, LIMIT)
        active = (glu * jax.nn.sigmoid(SLOPE * glu) * (linear + 1.0)).astype(jnp.bfloat16)
        output = jnp.zeros((buffer.shape[0], width), jnp.float32)
        for index in range(N_TP):
            output = output + rounded(jnp.dot(active[:, index * piece_size:(index + 1) * piece_size], down_weight[index * piece_size:(index + 1) * piece_size], preferred_element_type=jnp.float32))
        return output.astype(jnp.bfloat16)
    outputs = lax.map(expert_apply, (picks, expert_gate_weight, expert_linear_weight, expert_down_weight))
    outputs = jnp.transpose(outputs.reshape(EXPERTS, blocks, CAP, width), (1, 0, 2, 3)).reshape(blocks, EXPERTS * CAP, width)
    picked = jnp.take_along_axis(outputs, slots[:, :, None], axis=1)
    picked = picked.astype(jnp.float32).reshape(tokens, TOPK, width)
    routed = lax.optimization_barrier(jnp.sum(picked * routing_weight[:, :, None], axis=1))
    return (middle_wide + routed).astype(jnp.bfloat16)
```

```python
import functools
import math

import jax
import jax.numpy as jnp
from jax import lax
from jax.experimental import pallas as pl
from jax.experimental.pallas import tpu as pltpu
from jax.sharding import Mesh
from jax.sharding import PartitionSpec as P

SP = ("sp_0", "sp_1", "sp_2")
SP_TP = ("sp_0", "sp_1", "sp_2", "tp")

EPSILON = 1e-06
FLOOR_LOG = -1e30
LIMIT = 7.0
SLOPE = 1.702
HIGHEST = lax.Precision.HIGHEST
F32 = jnp.float32
BF16 = jnp.bfloat16

DKA, DVA, DKB, DVB = 128, 256, 64, 128
HEADS = 3
SLICE = 6
WEIGHT_PAIRS = [(0, 3), (3, 0), (1, 2), (2, 1)]
ROW_PAIRS = [(0, 1), (1, 0), (2, 3), (3, 2)]


def lane_scan(x, combine, identity):
    length = x.shape[1]
    lane = lax.broadcasted_iota(jnp.int32, x.shape, 1)
    step = 1
    while step < length:
        shifted = pltpu.roll(x, step, 1)
        x = combine(x, jnp.where(lane >= step, shifted, identity))
        step *= 2
    return x


def local_kernel(bk, bv, big, bfl, bfb, sk, sv, sig, sfl, sfb, out, rows, cols, gates, flat):
    length = bk.shape[0]
    gates[...] = jnp.zeros_like(gates)
    for at, (broad, slim) in enumerate(((big, sig), (bfl, sfl), (bfb, sfb))):
        gates[8 * at : 8 * at + 1, :] = broad[...]
        gates[8 * at + 1 : 8 * at + 3, :] = slim[...]
    forget = gates[8:16, :]
    logf = -(jnp.maximum(-forget, 0.0) + jnp.log1p(jnp.exp(-jnp.abs(forget)))) + gates[16:24, :]
    prefix = lane_scan(logf, jnp.add, 0.0)
    level = gates[0:8, :] - prefix
    peak = lane_scan(level, jnp.maximum, -jnp.inf)
    totals = prefix[:, length - 1 : length]
    top = peak[:, length - 1 : length]
    rows[...] = level
    cols[:, 0:8] = jnp.transpose(level)
    cols[:, 8:16] = jnp.transpose(peak)
    weights = jnp.transpose(jnp.exp(level - top))
    kw = (weights[:, 0:1] * (bk[...].astype(F32) * (1.0 / math.sqrt(DKA)))).astype(BF16)
    contract = (((0,), (0,)), ((), ()))
    memory = lax.dot_general(kw, bv[...], contract, preferred_element_type=F32)
    flat[0:128, :] = memory[:, 0:128]
    flat[128:256, :] = memory[:, 128:256]
    first = lax.broadcasted_iota(jnp.int32, sk.shape, 1) < DKB
    both = jnp.where(first, weights[:, 1:2], weights[:, 2:3])
    kw = (both * (sk[...].astype(F32) * (1.0 / math.sqrt(DKB)))).astype(BF16)
    memory = lax.dot_general(kw, sv[...], contract, preferred_element_type=F32)
    flat[256:320, :] = memory[0:64, 0:128]
    flat[320:384, :] = memory[64:128, 128:256]
    ends = jnp.concatenate([totals, totals + top, jnp.zeros((8, 126), F32)], axis=1)
    line = jnp.zeros((1, 128), F32)
    lane = lax.broadcasted_iota(jnp.int32, (1, 128), 1)
    for h in range(HEADS):
        line = jnp.where(lane == h, ends[h : h + 1, 0:1], line)
        line = jnp.where(lane == 3 + h, ends[h : h + 1, 1:2], line)
    tail = jnp.concatenate([line, jnp.zeros((1, 128), F32)], axis=0)
    for p in range(out.shape[0]):
        out[p, 0:SLICE, :] = flat[SLICE * p : SLICE * p + SLICE, :]
        out[p, SLICE:8, :] = tail


def scan_kernel(place, arrived, out):
    count = arrived.shape[0]
    sub = lax.broadcasted_iota(jnp.int32, (8, 128), 0)
    row = sub + SLICE * place[0]
    is_first, is_second = (row < 256, row < 320)
    lane = lax.broadcasted_iota(jnp.int32, (8, 128), 1)

    def spread(line, at):
        return jnp.where(
            is_first,
            line[:, at : at + 1],
            jnp.where(is_second, line[:, at + 1 : at + 2], line[:, at + 2 : at + 3]),
        )

    memory = jnp.zeros((8, 128), F32)
    level = jnp.full((8, 128), FLOOR_LOG, F32)
    levels = [jnp.full((1, 1), FLOOR_LOG, F32) for _ in range(HEADS)]
    for s in range(count):
        tail = jnp.where(
            lane == 0, levels[0], jnp.where(lane == 1, levels[1], levels[2])
        )
        out[s] = jnp.where(sub < SLICE, memory, tail)
        if s == count - 1:
            break
        line = arrived[s, SLICE : SLICE + 1, :]
        total, local = (spread(line, 0), spread(line, 3))
        later = jnp.maximum(total + level, local)
        memory = jnp.exp(total + level - later) * memory + jnp.exp(local - later) * arrived[s]
        level = later
        levels = [
            jnp.maximum(line[:, h : h + 1] + levels[h], line[:, 3 + h : 4 + h])
            for h in range(HEADS)
        ]


def inside_kernel(bq, bk, bv, sq, sk, sv, rows, cols, routes, out, slots):
    length = bq.shape[0]
    first = lax.broadcasted_iota(jnp.int32, sq.shape, 1) < DKB
    zero = jnp.zeros_like(sq)
    groups = (
        (bq[...], bk, bv, 0, DVA, math.sqrt(DKA)),
        (jnp.where(first, sq[...], zero), sk, sv, 0, DVB, math.sqrt(DKB)),
        (jnp.where(first, zero, sq[...]), sk, sv, DVB, DVB, math.sqrt(DKB)),
    )
    step = 128
    at = 0
    for h, (query, key, value, offset, width, root) in enumerate(groups):
        for i in range(length // step):
            upto = step * (i + 1)
            mine = slice(step * i, upto)
            scores = lax.dot_general(
                query[mine, :], key[0:upto, :], (((1,), (1,)), ((), ())), preferred_element_type=F32
            )
            gap = rows[h : h + 1, 0:upto] - cols[mine, 8 + h : 9 + h]
            t = lax.broadcasted_iota(jnp.int32, (step, upto), 0) + step * i
            s = lax.broadcasted_iota(jnp.int32, (step, upto), 1)
            decay = jnp.exp(jnp.where(t >= s, gap, -jnp.inf))
            chosen = (decay * (scores * (1.0 / root))).astype(BF16)
            out[mine, at : at + width] = jnp.dot(
                chosen, value[0:upto, offset : offset + width], preferred_element_type=F32
            )
        at += width
    count = routes.shape[0]
    experts = lax.broadcasted_iota(jnp.int32, (count, 128), 1)
    one = (routes[:, 0:1] == experts).astype(F32)
    two = (routes[:, 1:2] == experts).astype(F32)
    lower = (
        lax.broadcasted_iota(jnp.int32, (count, count), 0)
        > lax.broadcasted_iota(jnp.int32, (count, count), 1)
    ).astype(BF16)
    before = jnp.dot(lower, one.astype(BF16), preferred_element_type=F32)
    rank = jnp.sum(before * one, axis=1, keepdims=True).astype(jnp.int32)
    slots[:, 0:1] = routes[:, 0:1] * 8 + rank
    before = jnp.dot(lower, two.astype(BF16), preferred_element_type=F32)
    before = before + jnp.sum(one, axis=0, keepdims=True)
    rank = jnp.sum(before * two, axis=1, keepdims=True).astype(jnp.int32)
    slots[:, 1:2] = routes[:, 1:2] * 8 + rank


def read_kernel(state, cols, inside, bq, sq, bgate, sgate, bweight, sweight, out, flat, mixed):
    for p in range(state.shape[0]):
        flat[SLICE * p : SLICE * p + SLICE, :] = state[p, 0:SLICE, :]
    line = state[0, SLICE : SLICE + 1, :]
    first = lax.broadcasted_iota(jnp.int32, sq.shape, 1) < DKB
    wide = sq[...].astype(F32)
    query = bq[...].astype(F32)
    broad = jnp.concatenate(
        [
            jnp.dot(query, flat[0:128, :], precision=HIGHEST, preferred_element_type=F32),
            jnp.dot(query, flat[128:256, :], precision=HIGHEST, preferred_element_type=F32),
        ],
        axis=1,
    )
    both = flat[256:384, :]
    carried = (
        broad,
        jnp.dot(
            jnp.where(first, wide, 0.0), both, precision=HIGHEST, preferred_element_type=F32
        ),
        jnp.dot(
            jnp.where(first, 0.0, wide), both, precision=HIGHEST, preferred_element_type=F32
        ),
    )
    gates = (bgate[...], sgate[:, 0:DVB], sgate[:, DVB : 2 * DVB])
    at = 0
    for h in range(HEADS):
        width = carried[h].shape[1]
        peak = cols[:, 8 + h : 9 + h]
        level = line[:, h : h + 1]
        top = jnp.maximum(level, peak)
        cell = jnp.exp(level - top) * carried[h] + jnp.exp(peak - top) * inside[:, at : at + width]
        square = jnp.mean(cell * cell, axis=1, keepdims=True)
        normed = cell * lax.rsqrt(square + EPSILON)
        mixed[:, at : at + width] = (normed * jax.nn.sigmoid(gates[h].astype(F32))).astype(BF16)
        at += width
    out[...] = (
        jnp.dot(mixed[:, 0:DVA], bweight[...], preferred_element_type=F32)
        + jnp.dot(mixed[:, DVA : 2 * DVA], sweight[...], preferred_element_type=F32)
    ).astype(BF16)


def middle_kernel(stream, parts, gain, slots, middle, outgoing):
    total = parts[0].astype(F32)
    for j in range(1, parts.shape[0]):
        total = total + parts[j].astype(F32)
    rounded = (stream[...].astype(F32) + total).astype(BF16)
    middle[...] = rounded
    wide = rounded.astype(F32)
    square = jnp.mean(wide * wide, axis=1, keepdims=True)
    normed = (wide * lax.rsqrt(square + EPSILON) * gain[...]).astype(BF16)
    count = normed.shape[0]
    lane = lax.broadcasted_iota(jnp.int32, (count, outgoing.shape[0]), 1)
    named = jnp.logical_or(slots[:, 0:1] == lane, slots[:, 1:2] == lane)
    outgoing[...] = lax.dot_general(
        named.astype(F32).astype(BF16),
        normed,
        (((0,), (0,)), ((), ())),
        preferred_element_type=F32,
    ).astype(BF16)


def combine_kernel(middle, returned, slots, weight, out):
    count = middle.shape[0]
    lane = lax.broadcasted_iota(jnp.int32, (count, returned.shape[0]), 1)
    total = jnp.zeros(middle.shape, F32)
    for k in range(2):
        picked = jnp.dot(
            (slots[:, k : k + 1] == lane).astype(F32).astype(BF16),
            returned[...],
            preferred_element_type=F32,
        )
        total = total + picked * weight[:, k : k + 1]
    out[...] = (middle[...].astype(F32) + total).astype(BF16)


def shape(dims, dtype):
    return jax.ShapeDtypeStruct(dims, dtype)


def activation(rows, gate_weight, linear_weight):
    gate_pre = jnp.dot(rows, gate_weight, preferred_element_type=F32)
    lin_pre = jnp.dot(rows, linear_weight, preferred_element_type=F32)
    glu = jnp.minimum(gate_pre, LIMIT)
    linear = jnp.clip(lin_pre, -LIMIT, LIMIT)
    return (glu * jax.nn.sigmoid(SLOPE * glu) * (linear + 1.0)).astype(BF16)


def on_device(
    stream,
    broad_queries,
    broad_keys,
    broad_values,
    broad_output_gate,
    broad_input_gate,
    broad_forget_logits,
    broad_forget_boost,
    slim_queries,
    slim_keys,
    slim_values,
    slim_output_gate,
    slim_input_gate,
    slim_forget_logits,
    slim_forget_boost,
    broad_output_weight,
    slim_output_weight,
    expert_norm_gain,
    routes,
    routing_weight,
    expert_gate_weight,
    expert_linear_weight,
    expert_down_weight,
):
    count = lax.axis_size(SP)
    tp_count = lax.axis_size("tp")
    place = lax.axis_index(SP)
    own = lax.axis_index("tp")
    length = broad_queries.shape[0]
    rows, width = stream.shape
    capacity = 8

    gate_own, linear_own = (expert_gate_weight[0], expert_linear_weight[0])
    gate_other = lax.ppermute(gate_own, "tp", WEIGHT_PAIRS)
    linear_other = lax.ppermute(linear_own, "tp", WEIGHT_PAIRS)
    down_all = lax.all_gather(expert_down_weight, "tp", axis=0, tiled=True)

    payload, level_rows, level_cols = pl.pallas_call(
        local_kernel,
        out_shape=(
            shape((count, 8, 128), F32),
            shape((8, length), F32),
            shape((length, 16), F32),
        ),
        scratch_shapes=[pltpu.VMEM((24, length), F32), pltpu.VMEM((SLICE * 64, 128), F32)],
        name="local",
    )(
        broad_keys,
        broad_values,
        broad_input_gate,
        broad_forget_logits,
        broad_forget_boost,
        slim_keys,
        slim_values,
        slim_input_gate,
        slim_forget_logits,
        slim_forget_boost,
    )
    arrived = lax.all_to_all(payload, SP, split_axis=0, concat_axis=0, tiled=True)
    own_routes = lax.dynamic_slice_in_dim(routes, own * rows, rows, 0)
    inside, slots = pl.pallas_call(
        inside_kernel,
        out_shape=(shape((length, 512), F32), shape((rows, 2), jnp.int32)),
        name="inside",
    )(
        broad_queries,
        broad_keys,
        broad_values,
        slim_queries,
        slim_keys,
        slim_values,
        level_rows,
        level_cols,
        own_routes,
    )
    entering = pl.pallas_call(
        scan_kernel,
        out_shape=shape((count, 8, 128), F32),
        in_specs=[
            pl.BlockSpec(memory_space=pltpu.SMEM),
            pl.BlockSpec(memory_space=pltpu.VMEM),
        ],
        name="scan",
    )(place.reshape(1), arrived)
    state = lax.all_to_all(entering, SP, split_axis=0, concat_axis=0, tiled=True)
    part = pl.pallas_call(
        read_kernel,
        out_shape=shape((length, width), BF16),
        scratch_shapes=[pltpu.VMEM((SLICE * 64, 128), F32), pltpu.VMEM((length, 512), BF16)],
        name="read",
    )(
        state,
        level_cols,
        inside,
        broad_queries,
        slim_queries,
        broad_output_gate,
        slim_output_gate,
        broad_output_weight,
        slim_output_weight,
    )
    parts = lax.all_to_all(
        part.reshape(tp_count, rows, width), "tp", split_axis=0, concat_axis=0, tiled=True
    )
    middle, outgoing = pl.pallas_call(
        middle_kernel,
        out_shape=(shape((rows, width), BF16), shape((count * capacity, width), BF16)),
        name="middle",
    )(stream, parts, expert_norm_gain.reshape(1, width), slots)
    dispatched = lax.all_to_all(
        outgoing.reshape(count, capacity, width), SP, split_axis=0, concat_axis=0, tiled=True
    ).reshape(count * capacity, width)
    partner_rows = lax.ppermute(dispatched, "tp", ROW_PAIRS)
    sent = jnp.stack(
        [
            activation(partner_rows, gate_own, linear_own),
            activation(partner_rows, gate_other, linear_other),
        ]
    )
    received = lax.ppermute(sent, "tp", ROW_PAIRS)
    mine = (
        activation(dispatched, gate_own, linear_own),
        activation(dispatched, gate_other, linear_other),
    )
    other = own ^ 1
    out = (
        jnp.dot(mine[0], expert_down_weight[0], preferred_element_type=F32)
        + jnp.dot(
            mine[1],
            lax.dynamic_index_in_dim(down_all, 3 - own, 0, keepdims=False),
            preferred_element_type=F32,
        )
        + jnp.dot(
            received[0],
            lax.dynamic_index_in_dim(down_all, other, 0, keepdims=False),
            preferred_element_type=F32,
        )
        + jnp.dot(
            received[1],
            lax.dynamic_index_in_dim(down_all, 3 - other, 0, keepdims=False),
            preferred_element_type=F32,
        )
    ).astype(BF16)
    returned = lax.all_to_all(
        out.reshape(count, capacity, width), SP, split_axis=0, concat_axis=0, tiled=True
    ).reshape(count * capacity, width)
    return pl.pallas_call(
        combine_kernel, out_shape=shape((rows, width), BF16), name="combine"
    )(middle, returned, slots, routing_weight)


def solution(mesh):
    finer = Mesh(mesh.devices.reshape(8, 4, 2, mesh.shape["tp"]), ("sp_0", "sp_1", "sp_2", "tp"))
    in_specs = (
        P(SP_TP, None),
        P(SP, "tp"),
        P(SP, "tp"),
        P(SP, "tp"),
        P(SP, "tp"),
        P("tp", SP),
        P("tp", SP),
        P("tp", SP),
        P(SP, "tp"),
        P(SP, "tp"),
        P(SP, "tp"),
        P(SP, "tp"),
        P("tp", SP),
        P("tp", SP),
        P("tp", SP),
        P("tp", None),
        P("tp", None),
        P(),
        P(SP, None),
        P(SP_TP, None),
        P(SP, None, "tp"),
        P(SP, None, "tp"),
        P(SP, "tp", None),
    )
    out_specs = P(SP_TP, None)
    return jax.shard_map(
        on_device, mesh=finer, in_specs=in_specs, out_specs=out_specs, check_vma=False
    )
```
